512 devices in a mesh: sp: 32 (over z, x), dp: 16 (over y, core).
Axes of the slice: x: 4, y: 8, z: 8, core: 2. Of those that a mesh axis runs over, the one named last changes fastest.
Arguments:
- queries: bfloat16 [16, 4096, 2048], P('dp', 'sp'), may hold values from -6 to 6
- keys: bfloat16 [16, 4096, 2048], P('dp', 'sp'), may hold values from -6 to 6
- values: bfloat16 [16, 4096, 2048], P('dp', 'sp'), may hold values from -6 to 6
- gate_totals: float32 [16, 4096, 32], P('dp', 'sp'), may hold values from -4096 to 0, as said below
- w_out: bfloat16 [2048, 2048], P(None, 'dp'), may hold values from -1 to 1
Outputs:
- mixed: bfloat16 [16, 4096, 2048], P('dp', 'sp')
The draws below stay inside these ranges and needn't reach their ends.
Inputs may be any that keep to these rules, and one draw needn't show every extreme that they name: `gate_totals`: never rising along a sequence.
All inputs are finite; a program needn't handle non-finite values.
Results may differ from the reference program's by a relative error of at most 0.0053.
Values may be sent and summed in bfloat16 or wider, within the bound.
No kernel may reach another device: no remote copies, remote signals or barrier semaphores. Data moves between devices by JAX's collectives and lax.ppermute only.
A program may use at most 64 MiB of HBM per device.

```python
import math
import jax
import jax.numpy as jnp
from jax import lax

D = 2048
HEADS = 32
HEAD_DIM = 64
ATTN = 2048
LENGTH = 4096
BATCH = 16


def paired_draw(key):
    base = jax.random.fold_in(key, 11)
    first, second = jax.random.split(base, 2)
    shape = (BATCH, LENGTH, ATTN)
    query_draw = jnp.clip(jax.random.normal(first, shape, jnp.float32), -6.0, 6.0)
    key_draw = jnp.clip(jax.random.normal(second, shape, jnp.float32), -6.0, 6.0)
    return (query_draw, key_draw)


def draw_queries(key, part):
    return paired_draw(key)[0].astype(jnp.bfloat16)


def draw_keys(key, part):
    return paired_draw(key)[1].astype(jnp.bfloat16)


def draw_gate_totals(key, part):
    base = jax.random.fold_in(key, 23)
    first, second, third = jax.random.split(base, 3)
    fast_share = 0.5
    fast_heads = jax.random.bernoulli(first, fast_share, (BATCH, 1, HEADS))
    rates = jnp.where(fast_heads, 0.075, 1.2 / LENGTH).astype(jnp.float32)
    rough = jax.random.uniform(second, (BATCH, LENGTH, HEADS), jnp.float32, 0.3, 1.7)
    blocks = (LENGTH + 63) // 64
    block_scale = jnp.exp(jax.random.uniform(third, (BATCH, blocks, 1), jnp.float32, math.log(0.4), math.log(2.5)))
    block_scale = jnp.repeat(block_scale, 64, axis=1)[:, :LENGTH]
    log_gates = -rates * rough * block_scale
    return jnp.cumsum(log_gates, axis=1)


def level_of(stream_key, shape, cuts, least, top_value):
    level = 1.0
    for axis_at, parts in cuts:
        heights = jax.random.uniform(jax.random.fold_in(jax.random.fold_in(stream_key, 6), axis_at), (parts,), jnp.float32, least / len(cuts), top_value / len(cuts))
        level = level * jnp.repeat(jnp.exp(heights), shape[axis_at] // parts).reshape((-1,) + (1,) * (len(shape) - 1 - axis_at))
    return level


def bell_draw(stream_key, extent, width, bound, cuts=(), dtype=jnp.bfloat16):
    gain = level_of(stream_key, extent, cuts, -0.22, 0.18) if cuts else 1.0
    drawn = jax.random.normal(stream_key, extent, jnp.float32) * width * gain
    return jnp.minimum(jnp.maximum(drawn, -bound), bound).astype(dtype)


def setup_inputs(seed: int = 0) -> dict:
    splits = jax.random.split(jax.random.key(seed), 6)
    return {
        "queries": draw_queries(jax.random.fold_in(splits[5], 71), 0),
        "keys": draw_keys(jax.random.fold_in(splits[5], 71), 0),
        "values": bell_draw(splits[2], (BATCH, LENGTH, ATTN), 1.0, 6.0, ((0, 16), (1, 32))),
        "gate_totals": draw_gate_totals(jax.random.fold_in(splits[5], 71), 0),
        "w_out": bell_draw(splits[4], (ATTN, D), HEADS ** -0.5, 1.0, ((1, 16),)),
    }


def attend(queries, key_rows, value_rows, totals):
    length = queries.shape[0]
    block_rows = min(length, 512)
    pieces = []
    for begin_row in range(0, length, block_rows):
        end_row = begin_row + block_rows
        scores = jnp.einsum('qhd,khd->hqk', queries[begin_row:end_row].astype(jnp.float32), key_rows[:end_row].astype(jnp.float32)) * HEAD_DIM ** -0.5
        scores = scores + jnp.transpose(totals[begin_row:end_row])[:, :, None] - jnp.transpose(totals[:end_row])[:, None, :]
        causal = jnp.arange(end_row)[None, :] <= (begin_row + jnp.arange(block_rows))[:, None]
        scores = jnp.where(causal[None], scores, -jnp.inf)
        biggest = jnp.max(scores, axis=-1, keepdims=True)
        expo = jnp.exp(scores - biggest)
        summed = jnp.sum(expo, axis=-1)
        weights = expo.astype(jnp.bfloat16).astype(jnp.float32)
        output = jnp.einsum('hqk,khd->qhd', weights, value_rows[:end_row].astype(jnp.float32))
        output = output / jnp.transpose(summed)[:, :, None]
        pieces.append(output.astype(jnp.bfloat16))
    return jnp.concatenate(pieces, axis=0).reshape(length, -1)


def reference(queries, keys, values, gate_totals, w_out):
    shape4 = (BATCH, LENGTH, HEADS, HEAD_DIM)

    def one_sequence(items):
        return attend(items[0], items[1], items[2], items[3])

    attended = lax.map(one_sequence, (queries.reshape(shape4), keys.reshape(shape4), values.reshape(shape4), gate_totals))
    mixed = jnp.dot(attended.reshape(BATCH * LENGTH, ATTN), w_out, preferred_element_type=jnp.float32)
    return mixed.astype(jnp.bfloat16).reshape(BATCH, LENGTH, D)
```

```python
import functools
import math

import jax
import jax.numpy as jnp
from jax import lax
from jax.experimental import pallas as pl
from jax.experimental.pallas import tpu as pltpu
from jax.sharding import Mesh
from jax.sharding import PartitionSpec as P

HD = 64
SP = ("sp_0", "sp_1")
LOG2E = math.log2(math.e)
F32 = jnp.float32
BF16 = jnp.bfloat16
TILE = 128
ROWS = 208
BLK = 512


def split3(x):
    a = x.astype(BF16)
    r = x - a.astype(F32)
    b = r.astype(BF16)
    c = (r - b.astype(F32)).astype(BF16)
    return a, b, c


def gate_rows(a, b, c):
    row = lax.broadcasted_iota(jnp.int32, (16, a.shape[1]), 0)
    a, b, c = (t.astype(F32) for t in (a, b, c))
    t = jnp.where(row == 0, a, jnp.where(row == 1, b, jnp.where(row == 2, c, 0.0)))
    return t.astype(BF16)


def pack_kernel(q_ref, k_ref, v_ref, g_ref, o_ref):
    heads = o_ref.shape[0]
    a, b, c = split3(jnp.transpose(g_ref[0]))
    a, b, c = (t.astype(F32) for t in (a, b, c))
    for p in range(heads // 2):
        cols = slice(2 * p * HD, 2 * (p + 1) * HD)
        for ref, at in ((k_ref, 0), (q_ref, 80), (v_ref, 144)):
            t = jnp.transpose(ref[0, :, cols])
            o_ref[2 * p, at : at + HD, :] = t[:HD]
            o_ref[2 * p + 1, at : at + HD, :] = t[HD:]
    for h in range(heads):
        o_ref[h, 64:80, :] = gate_rows(a[h : h + 1], b[h : h + 1], c[h : h + 1])


def pack(q, k, v, g):
    heads = q.shape[2] // HD
    vm = pl.BlockSpec(memory_space=pltpu.VMEM)
    return pl.pallas_call(
        pack_kernel,
        out_shape=jax.ShapeDtypeStruct((heads, ROWS, q.shape[1]), BF16),
        in_specs=[vm] * 4,
        out_specs=vm,
        cost_estimate=pl.CostEstimate(flops=10**7, bytes_accessed=4 * 10**6, transcendentals=0),
        name="pack",
    )(q, k, v, g)


def attend_kernel(r_ref, o_ref, kaug, qaug, vaug, s0, s1, acc, cref):
    nb = kaug.shape[0]
    per = BLK // TILE

    rows64 = lax.broadcasted_iota(jnp.int32, (64, BLK), 0)
    ones_rows = jnp.where(rows64 < 3, 1.0, 0.0).astype(BF16)
    vrow = lax.broadcasted_iota(jnp.int32, (16, BLK), 0)
    vones = jnp.where(vrow < 1, 1.0, 0.0).astype(BF16)

    def prepare(c, _):
        gs = []
        for t in range(per):
            g = r_ref[c * per + t, 64:80, :].astype(F32)
            gs.append(g[0:1] + g[1:2] + g[2:3])
        ref = jnp.broadcast_to(gs[-1][:, TILE - 1 : TILE], (1, TILE))
        cref[c] = jnp.broadcast_to(jnp.concatenate([ref * LOG2E] * per, axis=1), (8, BLK))
        for t in range(per):
            j = c * per + t
            lanes = slice(t * TILE, (t + 1) * TILE)
            kt = r_ref[j, 0:64, :]
            bias = gate_rows(*split3((ref - gs[t]) * LOG2E))
            lo = jnp.concatenate([kt, kt], axis=0)
            hi = jnp.concatenate([kt, bias, jnp.zeros((48, TILE), BF16)], axis=0)
            kaug[c, lanes, 0:128] = jnp.transpose(lo)
            kaug[c, lanes, 128:256] = jnp.transpose(hi)
            q1, q2, q3 = split3(r_ref[j, 80:144, :].astype(F32) * (LOG2E * HD**-0.5))
            qaug[c, 0:64, lanes] = q1
            qaug[c, 64:128, lanes] = q2
            qaug[c, 128:192, lanes] = q3
            vaug[c, 0:64, lanes] = r_ref[j, 144:208, :]
        qaug[c, 192:256, :] = ones_rows
        vaug[c, 64:80, :] = vones
        return 0

    lax.fori_loop(0, nb, prepare, 0)

    def fold(s):
        return jnp.max(s.reshape(BLK // 8, 8, BLK), axis=0)

    def scores(i, c):
        return jnp.dot(kaug[c], qaug[i], preferred_element_type=F32)

    def diagonal(i, dst):
        s = scores(i, i)
        key = lax.broadcasted_iota(jnp.int32, (BLK, BLK), 0)
        query = lax.broadcasted_iota(jnp.int32, (BLK, BLK), 1)
        s = jnp.where(key <= query, s, -jnp.inf)
        dst[i] = s
        return fold(s)

    def weigh(c, m, src, i):
        mm = m - (cref[i] - cref[c])
        p = jnp.exp2(src[c].reshape(BLK // 8, 8, BLK) - mm[None])
        p = p.reshape(BLK, BLK).astype(BF16)
        return jnp.dot(vaug[c], p, preferred_element_type=F32)

    peak8 = diagonal(0, s0)
    for i in range(nb):
        src, dst = (s0, s1) if i % 2 == 0 else (s1, s0)
        m = jnp.broadcast_to(jnp.max(peak8, axis=0, keepdims=True), (8, BLK))
        acc[...] = jnp.zeros_like(acc)
        if i + 1 < nb:

            def both(c, peak, i=i, m=m, src=src, dst=dst):
                s = scores(i + 1, c)
                dst[c] = s
                peak = jnp.maximum(peak, fold(s) + (cref[i + 1] - cref[c]))
                acc[...] += weigh(c, m, src, i)
                return peak

            peak8 = lax.fori_loop(0, i + 1, both, jnp.full((8, BLK), -jnp.inf, F32))
            peak8 = jnp.maximum(peak8, diagonal(i + 1, dst))
        else:

            def last(c, _, i=i, m=m, src=src):
                acc[...] += weigh(c, m, src, i)
                return 0

            lax.fori_loop(0, i + 1, last, 0)
        out = (acc[0:64, :] / acc[64:65, :]).astype(BF16)
        for t in range(per):
            o_ref[i * per + t] = out[:, t * TILE : (t + 1) * TILE]


def attend(r):
    n = r.shape[0]
    length = n * TILE
    nb = length // BLK
    vm = pl.BlockSpec(memory_space=pltpu.VMEM)
    return pl.pallas_call(
        attend_kernel,
        out_shape=jax.ShapeDtypeStruct((n, HD, TILE), BF16),
        in_specs=[vm],
        out_specs=vm,
        scratch_shapes=[
            pltpu.VMEM((nb, BLK, 256), BF16),
            pltpu.VMEM((nb, 256, BLK), BF16),
            pltpu.VMEM((nb, 80, BLK), BF16),
            pltpu.VMEM((nb, BLK, BLK), F32),
            pltpu.VMEM((nb, BLK, BLK), F32),
            pltpu.VMEM((80, BLK), F32),
            pltpu.VMEM((nb, 8, BLK), F32),
        ],
        compiler_params=pltpu.CompilerParams(vmem_limit_bytes=40 * 1024 * 1024),
        cost_estimate=pl.CostEstimate(
            flops=2 * length * length * HD, bytes_accessed=3 * 10**6, transcendentals=length * length // 2
        ),
        name="attend",
    )(r)


def local(queries, keys, values, gate_totals, w_out):
    w = lax.all_gather(w_out, "dp", axis=1, tiled=True)
    packed = pack(queries, keys, values, gate_totals)
    held = lax.all_to_all(packed, SP, split_axis=0, concat_axis=0, tiled=True)
    out = attend(held)
    back = lax.all_to_all(out, SP, split_axis=0, concat_axis=0, tiled=True)
    attended = back.reshape(-1, back.shape[2])
    mixed = lax.dot_general(attended, w, (((0,), (0,)), ((), ())), preferred_element_type=F32)
    return mixed.astype(BF16)[None]


def solution(mesh):
    torus = Mesh(mesh.devices.reshape(8, 4, mesh.shape["dp"]), ("sp_0", "sp_1", "dp"))
    rows = P("dp", SP, None)
    return jax.shard_map(
        local, mesh=torus, in_specs=(rows, rows, rows, rows, P(None, "dp")), out_specs=rows, check_vma=False
    )
```

```python
import math

import jax
import jax.numpy as jnp
from jax import lax
from jax.experimental import pallas as pl
from jax.experimental.pallas import tpu as pltpu
from jax.sharding import Mesh
from jax.sharding import PartitionSpec as P

HD = 64
SP = ("sp_0", "sp_1")
LOG2E = math.log2(math.e)
F32 = jnp.float32
BF16 = jnp.bfloat16
TILE = 128
ROWS = 208
BLK = 512
SUB = 256
PARTS = 4
COLS = 8


def split3(x):
    a = x.astype(BF16)
    r = x - a.astype(F32)
    b = r.astype(BF16)
    c = (r - b.astype(F32)).astype(BF16)
    return a, b, c


def gate_rows(a, b, c):
    row = lax.broadcasted_iota(jnp.int32, (16, a.shape[1]), 0)
    a, b, c = (t.astype(F32) for t in (a, b, c))
    t = jnp.where(row == 0, a, jnp.where(row == 1, b, jnp.where(row == 2, c, 0.0)))
    return t.astype(BF16)


def pack_kernel(q_hbm, k_hbm, v_hbm, g_ref, o_hbm, buf, out, sems, osems):
    heads = out.shape[0]
    part = heads // PARTS
    width = part * HD
    sources = (k_hbm, q_hbm, v_hbm)

    def load(n, s):
        cols = slice(s * width, (s + 1) * width)
        return pltpu.make_async_copy(sources[n].at[0, :, cols], buf.at[n, :, cols], sems.at[n, s])

    def store(s):
        span = slice(s * part, (s + 1) * part)
        return pltpu.make_async_copy(out.at[span], o_hbm.at[span], osems.at[s])

    for s in range(PARTS):
        for n in range(3):
            load(n, s).start()
    a, b, c = (t.astype(F32) for t in split3(g_ref[0]))
    for h in range(heads):
        out[h, 64:80, :] = gate_rows(a[h : h + 1], b[h : h + 1], c[h : h + 1])
    for s in range(PARTS):
        for n, at in enumerate((0, 80, 144)):
            load(n, s).wait()
            for p in range(s * part // 2, (s + 1) * part // 2):
                t = jnp.transpose(buf[n, :, 2 * p * HD : 2 * (p + 1) * HD])
                out[2 * p, at : at + HD, :] = t[:HD]
                out[2 * p + 1, at : at + HD, :] = t[HD:]
        store(s).start()
    for s in range(PARTS):
        store(s).wait()


def pack(q, k, v, g):
    heads = q.shape[2] // HD
    hbm = pl.BlockSpec(memory_space=pl.ANY)
    vm = pl.BlockSpec(memory_space=pltpu.VMEM)
    shape = (heads, ROWS, q.shape[1])
    return pl.pallas_call(
        pack_kernel,
        out_shape=jax.ShapeDtypeStruct(shape, BF16),
        in_specs=[hbm] * 3 + [vm],
        out_specs=hbm,
        scratch_shapes=[
            pltpu.VMEM((3, q.shape[1], q.shape[2]), BF16),
            pltpu.VMEM(shape, BF16),
            pltpu.SemaphoreType.DMA((3, PARTS)),
            pltpu.SemaphoreType.DMA((PARTS,)),
        ],
        cost_estimate=pl.CostEstimate(flops=10**7, bytes_accessed=4 * 10**6, transcendentals=0),
        name="pack",
    )(q, k, v, jnp.swapaxes(g, 1, 2))


def attend_kernel(r_ref, o_ref, kaug, qaug, vaug, s0, s1, acc, cref):
    nb = kaug.shape[0]
    per = BLK // TILE

    rows64 = lax.broadcasted_iota(jnp.int32, (64, BLK), 0)
    ones_rows = jnp.where(rows64 < 3, 1.0, 0.0).astype(BF16)
    vrow = lax.broadcasted_iota(jnp.int32, (16, BLK), 0)
    vones = jnp.where(vrow < 1, 1.0, 0.0).astype(BF16)

    def prepare(c, _):
        gs = []
        for t in range(per):
            g = r_ref[c * per + t, 64:80, :].astype(F32)
            gs.append(g[0:1] + g[1:2] + g[2:3])
        ref = jnp.broadcast_to(gs[-1][:, TILE - 1 : TILE], (1, TILE))
        cref[c] = jnp.broadcast_to(jnp.concatenate([ref] * per, axis=1), (8, BLK))
        for t in range(per):
            j = c * per + t
            lanes = slice(t * TILE, (t + 1) * TILE)
            bias = gate_rows(*split3(ref - gs[t]))
            kt = jnp.concatenate([r_ref[j, 0:64, :], bias, jnp.zeros((48, TILE), BF16)], axis=0)
            kaug[c, lanes, :] = jnp.transpose(kt)
            qaug[c, 0:64, lanes] = r_ref[j, 80:144, :] * BF16(HD**-0.5)
            vaug[c, 0:64, lanes] = r_ref[j, 144:208, :]
        qaug[c, 64:128, :] = ones_rows
        vaug[c, 64:80, :] = vones
        return 0

    lax.fori_loop(0, nb, prepare, 0)

    NS = BLK // SUB

    def fold(s):
        return jnp.max(s.reshape(s.shape[0] // 8, 8, BLK), axis=0)

    def scores(i, c, h):
        return jnp.dot(kaug[c, h * SUB : (h + 1) * SUB, :], qaug[i], preferred_element_type=F32)

    def diagonal(i, dst, h):
        s = scores(i, i, h)
        key = lax.broadcasted_iota(jnp.int32, (SUB, BLK), 0) + h * SUB
        query = lax.broadcasted_iota(jnp.int32, (SUB, BLK), 1)
        s = jnp.where(key <= query, s, -jnp.inf)
        dst[i, h * SUB : (h + 1) * SUB, :] = s
        return fold(s)

    def below(i, c, dst, h):
        s = scores(i, c, h)
        dst[c, h * SUB : (h + 1) * SUB, :] = s
        return fold(s)

    def weigh(c, mm, src, h):
        p = jnp.exp2((src[c, h * SUB : (h + 1) * SUB, :].reshape(SUB // 8, 8, BLK) - mm[None]) * LOG2E)
        p = p.reshape(SUB, BLK).astype(BF16)
        return jnp.dot(vaug[c, :, h * SUB : (h + 1) * SUB], p, preferred_element_type=F32)

    def most(a, b):
        return b if a is None else jnp.maximum(a, b)

    peak8 = None
    for h in range(NS):
        peak8 = most(peak8, diagonal(0, s0, h))
    for i in range(nb):
        src, dst = (s0, s1) if i % 2 == 0 else (s1, s0)
        m = jnp.broadcast_to(jnp.max(peak8, axis=0, keepdims=True), (8, BLK))
        peak8 = None
        total = jnp.zeros(acc.shape, F32)
        for c in range(i + 1):
            mm = m - (cref[i] - cref[c])
            f = None
            for h in range(NS):
                if i + 1 < nb:
                    f = most(f, below(i + 1, c, dst, h))
                total = total + weigh(c, mm, src, h)
            if i + 1 < nb:
                peak8 = most(peak8, f + (cref[i + 1] - cref[c]))
        if i + 1 < nb:
            for h in range(NS):
                peak8 = most(peak8, diagonal(i + 1, dst, h))
        acc[...] = total
        out = (acc[0:64, :] / acc[64:65, :]).astype(BF16)
        for t in range(per):
            o_ref[i * per + t] = out[:, t * TILE : (t + 1) * TILE]


def attend(r):
    n = r.shape[0]
    length = n * TILE
    nb = length // BLK
    vm = pl.BlockSpec(memory_space=pltpu.VMEM)
    return pl.pallas_call(
        attend_kernel,
        out_shape=jax.ShapeDtypeStruct((n, HD, TILE), BF16),
        in_specs=[vm],
        out_specs=vm,
        scratch_shapes=[
            pltpu.VMEM((nb, BLK, 128), BF16),
            pltpu.VMEM((nb, 128, BLK), BF16),
            pltpu.VMEM((nb, 80, BLK), BF16),
            pltpu.VMEM((nb, BLK, BLK), F32),
            pltpu.VMEM((nb, BLK, BLK), F32),
            pltpu.VMEM((80, BLK), F32),
            pltpu.VMEM((nb, 8, BLK), F32),
        ],
        compiler_params=pltpu.CompilerParams(vmem_limit_bytes=40 * 1024 * 1024),
        cost_estimate=pl.CostEstimate(
            flops=2 * length * length * HD, bytes_accessed=3 * 10**6, transcendentals=length * length // 2
        ),
        name="attend",
    )(r)


def project_kernel(a_ref, w_hbm, o_ref, w, sems):
    width = w_hbm.shape[1] // COLS

    def load(s):
        cols = slice(s * width, (s + 1) * width)
        return pltpu.make_async_copy(w_hbm.at[:, cols], w.at[:, cols], sems.at[s])

    for s in range(COLS):
        load(s).start()
    att = jnp.transpose(a_ref[...].reshape(-1, TILE))
    for s in range(COLS):
        load(s).wait()
        cols = slice(s * width, (s + 1) * width)
        o_ref[0, :, cols] = jnp.dot(att, w[:, cols], preferred_element_type=F32).astype(BF16)


def project(attended, w):
    vm = pl.BlockSpec(memory_space=pltpu.VMEM)
    return pl.pallas_call(
        project_kernel,
        out_shape=jax.ShapeDtypeStruct((1, TILE, w.shape[1]), BF16),
        in_specs=[vm, pl.BlockSpec(memory_space=pl.ANY)],
        out_specs=vm,
        scratch_shapes=[pltpu.VMEM(w.shape, BF16), pltpu.SemaphoreType.DMA((COLS,))],
        cost_estimate=pl.CostEstimate(
            flops=2 * TILE * w.size, bytes_accessed=w.size * 2 + 10**6, transcendentals=0
        ),
        name="project",
    )(attended, w)


def local(queries, keys, values, gate_totals, w_out):
    w = lax.all_gather(w_out, "dp", axis=1, tiled=True)
    packed = pack(queries, keys, values, gate_totals)
    held = lax.all_to_all(packed, SP, split_axis=0, concat_axis=0, tiled=True)
    out = attend(held)
    back = lax.all_to_all(out, SP, split_axis=0, concat_axis=0, tiled=True)
    return project(back, w)


def solution(mesh):
    torus = Mesh(mesh.devices.reshape(8, 4, mesh.shape["dp"]), ("sp_0", "sp_1", "dp"))
    rows = P("dp", SP, None)
    return jax.shard_map(
        local, mesh=torus, in_specs=(rows, rows, rows, rows, P(None, "dp")), out_specs=rows, check_vma=False
    )
```

```python
import math

import jax
import jax.numpy as jnp
from jax import lax
from jax.experimental import pallas as pl
from jax.experimental.pallas import tpu as pltpu
from jax.sharding import Mesh
from jax.sharding import PartitionSpec as P

HD = 64
SP = ("sp_0", "sp_1")
LOG2E = math.log2(math.e)
F32 = jnp.float32
BF16 = jnp.bfloat16
TILE = 128
ROWS = 200
BLK = 512
SUB = 256
AHEAD = 6


def split3(x):
    a = x.astype(BF16)
    r = x - a.astype(F32)
    b = r.astype(BF16)
    c = (r - b.astype(F32)).astype(BF16)
    return a, b, c


def gate_rows(a, b, c):
    row = lax.broadcasted_iota(jnp.int32, (8, a.shape[1]), 0)
    a, b, c = (t.astype(F32) for t in (a, b, c))
    t = jnp.where(row == 0, a, jnp.where(row == 1, b, jnp.where(row == 2, c, 0.0)))
    return t.astype(BF16)


def pack_kernel(q_ref, k_ref, v_ref, g_ref, o_ref):
    heads = o_ref.shape[0]
    a, b, c = split3(g_ref[0])
    a, b, c = (t.astype(F32) for t in (a, b, c))
    for p in range(heads // 2):
        cols = slice(2 * p * HD, 2 * (p + 1) * HD)
        for ref, at in ((k_ref, 0), (q_ref, 64), (v_ref, 128)):
            t = jnp.transpose(ref[0, :, cols])
            o_ref[2 * p, at : at + HD, :] = t[:HD]
            o_ref[2 * p + 1, at : at + HD, :] = t[HD:]
    for h in range(heads):
        o_ref[h, 192:200, :] = gate_rows(a[h : h + 1], b[h : h + 1], c[h : h + 1])


def pack(q, k, v, g):
    heads = q.shape[2] // HD
    vm = pl.BlockSpec(memory_space=pltpu.VMEM)
    return pl.pallas_call(
        pack_kernel,
        out_shape=jax.ShapeDtypeStruct((heads, ROWS, q.shape[1]), BF16),
        in_specs=[vm] * 4,
        out_specs=vm,
        cost_estimate=pl.CostEstimate(flops=10**7, bytes_accessed=4 * 10**6, transcendentals=0),
        name="pack",
    )(q, k, v, jnp.swapaxes(g, 1, 2))


def attend_kernel(r_ref, o_ref, kaug, qaug, vaug, s0, s1, acc, cref):
    nb = kaug.shape[0]
    per = BLK // TILE

    rows64 = lax.broadcasted_iota(jnp.int32, (64, BLK), 0)
    ones_rows = jnp.where(rows64 < 3, 1.0, 0.0).astype(BF16)
    vrow = lax.broadcasted_iota(jnp.int32, (16, BLK), 0)
    vones = jnp.where(vrow < 1, 1.0, 0.0).astype(BF16)

    def prepare(c):
        gs = []
        for t in range(per):
            g = r_ref[c * per + t, 192:200, :].astype(F32)
            gs.append(g[0:1] + g[1:2] + g[2:3])
        ref = jnp.broadcast_to(gs[-1][:, TILE - 1 : TILE], (1, TILE))
        cref[c] = jnp.broadcast_to(jnp.concatenate([ref] * per, axis=1), (8, BLK))
        for t in range(per):
            j = c * per + t
            lanes = slice(t * TILE, (t + 1) * TILE)
            bias = gate_rows(*split3(ref - gs[t]))
            kt = jnp.concatenate([r_ref[j, 0:64, :], bias, jnp.zeros((56, TILE), BF16)], axis=0)
            kaug[c, lanes, :] = jnp.transpose(kt)
            qaug[c, 0:64, lanes] = r_ref[j, 64:128, :] * BF16(HD**-0.5)
            vaug[c, 0:64, lanes] = r_ref[j, 128:192, :]
        qaug[c, 64:128, :] = ones_rows
        vaug[c, 64:80, :] = vones

    prepare(0)
    prepare(1)

    NS = BLK // SUB

    def fold(s):
        return jnp.max(s.reshape(s.shape[0] // 8, 8, s.shape[1]), axis=0)

    def scores(i, c, h, at=0):
        return jnp.dot(kaug[c, h * SUB : (h + 1) * SUB, :], qaug[i, :, at:], preferred_element_type=F32)

    def diagonal(i, dst, h):
        at = 0
        s = scores(i, i, h, at)
        key = lax.broadcasted_iota(jnp.int32, s.shape, 0) + h * SUB
        query = lax.broadcasted_iota(jnp.int32, s.shape, 1)
        s = jnp.where(key <= query, s, -jnp.inf)
        dst[i, h * SUB : (h + 1) * SUB, :] = s
        f = fold(s)
        return f if at == 0 else jnp.concatenate([jnp.full((8, at), -jnp.inf, F32), f], axis=1)

    def below(i, c, dst, h):
        s = scores(i, c, h)
        dst[c, h * SUB : (h + 1) * SUB, :] = s
        return fold(s)

    def weigh(total, c, mm, src, h, at=0):
        width = BLK - at
        s = src[c, h * SUB : (h + 1) * SUB, at:].reshape(SUB // 8, 8, width)
        p = jnp.exp2((s - mm[None, :, at:]) * LOG2E).reshape(SUB, width).astype(BF16)
        part = jnp.dot(vaug[c, :, h * SUB : (h + 1) * SUB], p, preferred_element_type=F32)
        if at == 0:
            return total + part
        return jnp.concatenate([total[:, :at], total[:, at:] + part], axis=1)

    def most(a, b):
        return b if a is None else jnp.maximum(a, b)

    peak8 = None
    for h in range(NS):
        peak8 = most(peak8, diagonal(0, s0, h))
    for i in range(nb):
        src, dst = (s0, s1) if i % 2 == 0 else (s1, s0)
        m = jnp.broadcast_to(jnp.max(peak8, axis=0, keepdims=True), (8, BLK))
        peak8 = None
        if i + 2 < nb:
            prepare(i + 2)
        total = jnp.zeros(acc.shape, F32)
        for c in range(i + 1):
            mm = m - (cref[i] - cref[c])
            f = None
            for h in range(NS):
                if i + 1 < nb:
                    f = most(f, below(i + 1, c, dst, h))
                total = weigh(total, c, mm, src, h, 0)
            if i + 1 < nb:
                peak8 = most(peak8, f + (cref[i + 1] - cref[c]))
        if i + 1 < nb:
            for h in range(NS):
                peak8 = most(peak8, diagonal(i + 1, dst, h))
        acc[...] = total
        out = (acc[0:64, :] / acc[64:65, :]).astype(BF16)
        for t in range(per):
            o_ref[i * per + t] = out[:, t * TILE : (t + 1) * TILE]


def attend(r):
    n = r.shape[0]
    length = n * TILE
    nb = length // BLK
    vm = pl.BlockSpec(memory_space=pltpu.VMEM)
    return pl.pallas_call(
        attend_kernel,
        out_shape=jax.ShapeDtypeStruct((n, HD, TILE), BF16),
        in_specs=[vm],
        out_specs=vm,
        scratch_shapes=[
            pltpu.VMEM((nb, BLK, 128), BF16),
            pltpu.VMEM((nb, 128, BLK), BF16),
            pltpu.VMEM((nb, 80, BLK), BF16),
            pltpu.VMEM((nb, BLK, BLK), F32),
            pltpu.VMEM((nb, BLK, BLK), F32),
            pltpu.VMEM((80, BLK), F32),
            pltpu.VMEM((nb, 8, BLK), F32),
        ],
        compiler_params=pltpu.CompilerParams(vmem_limit_bytes=40 * 1024 * 1024),
        cost_estimate=pl.CostEstimate(
            flops=2 * length * length * HD, bytes_accessed=3 * 10**6, transcendentals=length * length // 2
        ),
        name="attend",
    )(r)


def project_kernel(a_hbm, w_hbm, o_hbm, a, w, o, asem, wsems, osems):
    pairs = w_hbm.shape[0] // 2

    def load(s):
        span = pl.ds(2 * s, 2)
        return pltpu.make_async_copy(w_hbm.at[span], w.at[span], wsems.at[s])

    def store(g):
        cols = slice(g * 512, (g + 1) * 512)
        return pltpu.make_async_copy(o.at[:, cols], o_hbm.at[0, :, cols], osems.at[g])

    first = pltpu.make_async_copy(a_hbm, a, asem)
    first.start()
    for s in range(AHEAD):
        load(s).start()
    first.wait()
    att = jnp.transpose(a[...].reshape(-1, TILE))
    for g in range(pairs // 2):
        for s in (2 * g, 2 * g + 1):
            load(s).wait()
            if s + AHEAD < pairs:
                load(s + AHEAD).start()
        quad = jnp.concatenate([w[4 * g + i] for i in range(4)], axis=1)
        o[:, g * 512 : (g + 1) * 512] = jnp.dot(att, quad, preferred_element_type=F32).astype(BF16)
        store(g).start()
    for g in range(pairs // 2):
        store(g).wait()


def project(attended, w):
    hbm = pl.BlockSpec(memory_space=pl.ANY)
    width = w.shape[0] * w.shape[2]
    pairs = w.shape[0] // 2
    return pl.pallas_call(
        project_kernel,
        out_shape=jax.ShapeDtypeStruct((1, TILE, width), BF16),
        in_specs=[hbm, hbm],
        out_specs=hbm,
        scratch_shapes=[
            pltpu.VMEM(attended.shape, BF16),
            pltpu.VMEM(w.shape, BF16),
            pltpu.VMEM((TILE, width), BF16),
            pltpu.SemaphoreType.DMA,
            pltpu.SemaphoreType.DMA((pairs,)),
            pltpu.SemaphoreType.DMA((pairs // 2,)),
        ],
        cost_estimate=pl.CostEstimate(
            flops=2 * TILE * w.size, bytes_accessed=w.size * 2 + 10**6, transcendentals=0
        ),
        name="project",
    )(attended, w)


def local(queries, keys, values, gate_totals, w_out):
    w = lax.all_gather(w_out, "dp", axis=0)
    packed = pack(queries, keys, values, gate_totals)
    held = lax.all_to_all(packed, SP, split_axis=0, concat_axis=0, tiled=True)
    out = attend(held)
    back = lax.all_to_all(out, SP, split_axis=0, concat_axis=0, tiled=True)
    return project(back, w)


def solution(mesh):
    torus = Mesh(mesh.devices.reshape(8, 4, mesh.shape["dp"]), ("sp_0", "sp_1", "dp"))
    rows = P("dp", SP, None)
    return jax.shard_map(
        local, mesh=torus, in_specs=(rows, rows, rows, rows, P(None, "dp")), out_specs=rows, check_vma=False
    )
```

```python
import math

import jax
import jax.numpy as jnp
from jax import lax
from jax.experimental import pallas as pl
from jax.experimental.pallas import tpu as pltpu
from jax.sharding import Mesh
from jax.sharding import PartitionSpec as P

HD = 64
SP = ("sp_0", "sp_1")
LOG2E = math.log2(math.e)
F32 = jnp.float32
BF16 = jnp.bfloat16
TILE = 128
ROWS = 200
BLK = 512
SUB = 256
AHEAD = 6


def split3(x):
    a = x.astype(BF16)
    r = x - a.astype(F32)
    b = r.astype(BF16)
    c = (r - b.astype(F32)).astype(BF16)
    return a, b, c


def gate_rows(a, b, c):
    row = lax.broadcasted_iota(jnp.int32, (8, a.shape[1]), 0)
    a, b, c = (t.astype(F32) for t in (a, b, c))
    t = jnp.where(row == 0, a, jnp.where(row == 1, b, jnp.where(row == 2, c, 0.0)))
    return t.astype(BF16)


def pack_kernel(q_hbm, k_hbm, v_hbm, g_hbm, o_hbm, buf, g, out, sems, osems):
    heads = out.shape[0]
    sources = (k_hbm, q_hbm, v_hbm)

    def load(n):
        return pltpu.make_async_copy(sources[n].at[0], buf.at[n], sems.at[n])

    def store(n):
        rows = slice(n * HD, (n + 1) * HD if n < 3 else ROWS)
        return pltpu.make_async_copy(out.at[:, rows, :], o_hbm.at[:, rows, :], osems.at[n])

    gates = pltpu.make_async_copy(g_hbm.at[0], g, sems.at[3])
    gates.start()
    for n in range(3):
        load(n).start()
    gates.wait()
    a, b, c = (t.astype(F32) for t in split3(g[...]))
    for h in range(heads):
        out[h, 192:200, :] = gate_rows(a[h : h + 1], b[h : h + 1], c[h : h + 1])
    store(3).start()
    for n in range(3):
        load(n).wait()
        for p in range(heads // 2):
            t = jnp.transpose(buf[n, :, 2 * p * HD : 2 * (p + 1) * HD])
            out[2 * p, n * HD : (n + 1) * HD, :] = t[:HD]
            out[2 * p + 1, n * HD : (n + 1) * HD, :] = t[HD:]
        store(n).start()
    for n in range(4):
        store(n).wait()


def pack(q, k, v, g):
    heads = q.shape[2] // HD
    hbm = pl.BlockSpec(memory_space=pl.ANY)
    shape = (heads, ROWS, q.shape[1])
    return pl.pallas_call(
        pack_kernel,
        out_shape=jax.ShapeDtypeStruct(shape, BF16),
        in_specs=[hbm] * 4,
        out_specs=hbm,
        scratch_shapes=[
            pltpu.VMEM((3, q.shape[1], q.shape[2]), BF16),
            pltpu.VMEM((heads, q.shape[1]), F32),
            pltpu.VMEM(shape, BF16),
            pltpu.SemaphoreType.DMA((4,)),
            pltpu.SemaphoreType.DMA((4,)),
        ],
        cost_estimate=pl.CostEstimate(flops=10**7, bytes_accessed=4 * 10**6, transcendentals=0),
        name="pack",
    )(q, k, v, jnp.swapaxes(g, 1, 2))


def attend_kernel(r_ref, o_ref, kaug, qaug, vaug, s0, s1, acc, cref):
    nb = kaug.shape[0]
    per = BLK // TILE

    rows64 = lax.broadcasted_iota(jnp.int32, (64, BLK), 0)
    ones_rows = jnp.where(rows64 < 3, 1.0, 0.0).astype(BF16)
    vrow = lax.broadcasted_iota(jnp.int32, (16, BLK), 0)
    vones = jnp.where(vrow < 1, 1.0, 0.0).astype(BF16)

    def prepare(c):
        gs = []
        for t in range(per):
            g = r_ref[c * per + t, 192:200, :].astype(F32)
            gs.append(g[0:1] + g[1:2] + g[2:3])
        ref = jnp.broadcast_to(gs[-1][:, TILE - 1 : TILE], (1, TILE))
        cref[c] = jnp.broadcast_to(jnp.concatenate([ref] * per, axis=1), (8, BLK))
        for t in range(per):
            j = c * per + t
            lanes = slice(t * TILE, (t + 1) * TILE)
            bias = gate_rows(*split3(ref - gs[t]))
            kt = jnp.concatenate([r_ref[j, 0:64, :], bias, jnp.zeros((56, TILE), BF16)], axis=0)
            kaug[c, lanes, :] = jnp.transpose(kt)
            qaug[c, 0:64, lanes] = r_ref[j, 64:128, :] * BF16(HD**-0.5)
            vaug[c, 0:64, lanes] = r_ref[j, 128:192, :]
        qaug[c, 64:128, :] = ones_rows
        vaug[c, 64:80, :] = vones

    prepare(0)
    prepare(1)

    NS = BLK // SUB

    def fold(s):
        return jnp.max(s.reshape(s.shape[0] // 8, 8, s.shape[1]), axis=0)

    def scores(i, c, h, at=0):
        return jnp.dot(kaug[c, h * SUB : (h + 1) * SUB, :], qaug[i, :, at:], preferred_element_type=F32)

    def diagonal(i, dst, h):
        at = 0
        s = scores(i, i, h, at)
        key = lax.broadcasted_iota(jnp.int32, s.shape, 0) + h * SUB
        query = lax.broadcasted_iota(jnp.int32, s.shape, 1)
        s = jnp.where(key <= query, s, -jnp.inf)
        dst[i, h * SUB : (h + 1) * SUB, :] = s
        f = fold(s)
        return f if at == 0 else jnp.concatenate([jnp.full((8, at), -jnp.inf, F32), f], axis=1)

    def below(i, c, dst, h):
        s = scores(i, c, h)
        dst[c, h * SUB : (h + 1) * SUB, :] = s
        return fold(s)

    def weigh(total, c, mm, src, h, at=0):
        width = BLK - at
        s = src[c, h * SUB : (h + 1) * SUB, at:].reshape(SUB // 8, 8, width)
        p = jnp.exp2((s - mm[None, :, at:]) * LOG2E).reshape(SUB, width).astype(BF16)
        part = jnp.dot(vaug[c, :, h * SUB : (h + 1) * SUB], p, preferred_element_type=F32)
        if at == 0:
            return total + part
        return jnp.concatenate([total[:, :at], total[:, at:] + part], axis=1)

    def most(a, b):
        return b if a is None else jnp.maximum(a, b)

    peak8 = None
    for h in range(NS):
        peak8 = most(peak8, diagonal(0, s0, h))
    for i in range(nb):
        src, dst = (s0, s1) if i % 2 == 0 else (s1, s0)
        m = jnp.broadcast_to(jnp.max(peak8, axis=0, keepdims=True), (8, BLK))
        peak8 = None
        if i + 2 < nb:
            prepare(i + 2)
        total = jnp.zeros(acc.shape, F32)
        for c in range(i + 1):
            mm = m - (cref[i] - cref[c])
            f = None
            for h in range(NS):
                if i + 1 < nb:
                    f = most(f, below(i + 1, c, dst, h))
                total = weigh(total, c, mm, src, h, 0)
            if i + 1 < nb:
                peak8 = most(peak8, f + (cref[i + 1] - cref[c]))
        if i + 1 < nb:
            for h in range(NS):
                peak8 = most(peak8, diagonal(i + 1, dst, h))
        acc[...] = total
        out = (acc[0:64, :] / acc[64:65, :]).astype(BF16)
        for t in range(per):
            o_ref[i * per + t] = out[:, t * TILE : (t + 1) * TILE]


def attend(r):
    n = r.shape[0]
    length = n * TILE
    nb = length // BLK
    vm = pl.BlockSpec(memory_space=pltpu.VMEM)
    return pl.pallas_call(
        attend_kernel,
        out_shape=jax.ShapeDtypeStruct((n, HD, TILE), BF16),
        in_specs=[vm],
        out_specs=vm,
        scratch_shapes=[
            pltpu.VMEM((nb, BLK, 128), BF16),
            pltpu.VMEM((nb, 128, BLK), BF16),
            pltpu.VMEM((nb, 80, BLK), BF16),
            pltpu.VMEM((nb, BLK, BLK), F32),
            pltpu.VMEM((nb, BLK, BLK), F32),
            pltpu.VMEM((80, BLK), F32),
            pltpu.VMEM((nb, 8, BLK), F32),
        ],
        compiler_params=pltpu.CompilerParams(vmem_limit_bytes=40 * 1024 * 1024),
        cost_estimate=pl.CostEstimate(
            flops=2 * length * length * HD, bytes_accessed=3 * 10**6, transcendentals=length * length // 2
        ),
        name="attend",
    )(r)


def project_kernel(a_hbm, w_hbm, o_hbm, a, w, o, asem, wsems, osems):
    pairs = w_hbm.shape[0] // 2

    def load(s):
        span = pl.ds(2 * s, 2)
        return pltpu.make_async_copy(w_hbm.at[span], w.at[span], wsems.at[s])

    def store(g):
        cols = slice(g * 512, (g + 1) * 512)
        return pltpu.make_async_copy(o.at[:, cols], o_hbm.at[0, :, cols], osems.at[g])

    first = pltpu.make_async_copy(a_hbm, a, asem)
    first.start()
    for s in range(AHEAD):
        load(s).start()
    first.wait()
    att = jnp.transpose(a[...].reshape(-1, TILE))
    for g in range(pairs // 2):
        for s in (2 * g, 2 * g + 1):
            load(s).wait()
            if s + AHEAD < pairs:
                load(s + AHEAD).start()
        quad = jnp.concatenate([w[4 * g + i] for i in range(4)], axis=1)
        o[:, g * 512 : (g + 1) * 512] = jnp.dot(att, quad, preferred_element_type=F32).astype(BF16)
        store(g).start()
    for g in range(pairs // 2):
        store(g).wait()


def project(attended, w):
    hbm = pl.BlockSpec(memory_space=pl.ANY)
    width = w.shape[0] * w.shape[2]
    pairs = w.shape[0] // 2
    return pl.pallas_call(
        project_kernel,
        out_shape=jax.ShapeDtypeStruct((1, TILE, width), BF16),
        in_specs=[hbm, hbm],
        out_specs=hbm,
        scratch_shapes=[
            pltpu.VMEM(attended.shape, BF16),
            pltpu.VMEM(w.shape, BF16),
            pltpu.VMEM((TILE, width), BF16),
            pltpu.SemaphoreType.DMA,
            pltpu.SemaphoreType.DMA((pairs,)),
            pltpu.SemaphoreType.DMA((pairs // 2,)),
        ],
        cost_estimate=pl.CostEstimate(
            flops=2 * TILE * w.size, bytes_accessed=w.size * 2 + 10**6, transcendentals=0
        ),
        name="project",
    )(attended, w)


def local(queries, keys, values, gate_totals, w_out):
    w = lax.all_gather(w_out, "dp", axis=0)
    packed = pack(queries, keys, values, gate_totals)
    held = lax.all_to_all(packed, SP, split_axis=0, concat_axis=0, tiled=True)
    out = attend(held)
    back = lax.all_to_all(out, SP, split_axis=0, concat_axis=0, tiled=True)
    return project(back, w)


def solution(mesh):
    torus = Mesh(mesh.devices.reshape(8, 4, mesh.shape["dp"]), ("sp_0", "sp_1", "dp"))
    rows = P("dp", SP, None)
    return jax.shard_map(
        local, mesh=torus, in_specs=(rows, rows, rows, rows, P(None, "dp")), out_specs=rows, check_vma=False
    )
```
